512 devices in a mesh: sp: 128 (over z, y, core), tp: 4 (over x).
Axes of the slice: x: 4, y: 8, z: 8, core: 2. Of those that a mesh axis runs over, the one named last changes fastest.
Arguments:
- tokens: bfloat16 [24576, 2048], P('sp'), may hold values from -10 to 10
- w_query: bfloat16 [2048, 1024], P(None, 'tp'), may hold values from -0.125 to 0.125
- w_key: bfloat16 [2048, 256], P(None, 'tp'), may hold values from -0.125 to 0.125
- w_value: bfloat16 [2048, 256], P(None, 'tp'), may hold values from -0.125 to 0.125
- w_output: bfloat16 [1024, 2048], P('tp'), may hold values from -0.1875 to 0.1875
- query_gain: float32 [64], replicated, may hold values from 0.4 to 9
- key_gain: float32 [64], replicated, may hold values from 0.4 to 9
Outputs:
- mixed_out: bfloat16 [24576, 2048], P(('sp', 'tp'))
- log_sums: float32 [16, 24576], P('tp', 'sp')
The draws below stay inside these ranges and needn't reach their ends.
All inputs are finite; a program needn't handle non-finite values.
Results may differ from the reference program's by a relative error of at most 0.009.
The reference program's roundings to bfloat16 on the way (of `weights` and `attended`) count: a program that leaves them out, or rounds other values in their place, can miss the bound.
Values may be sent and summed in bfloat16 or wider, within the bound.
A program may use at most 64 MiB of HBM per device.

```python
import math
import jax
import jax.numpy as jnp
from jax import lax

D = 2048
HEADS = 16
KV_HEADS = 4
HEAD = 64
GRID_W = 64
TOK_DEV = 192
TOKENS = 24576


def draw_tokens(key, part):
    first, second, third = jax.random.split(key, 3)
    n_blocks = TOKENS // TOK_DEV
    base = jax.random.normal(first, (TOKENS, D), jnp.float32)
    offsets = jax.random.uniform(second, (n_blocks, 1), jnp.float32, -0.5, 2.0)
    direction = jnp.clip(jax.random.normal(third, (1, D), jnp.float32), -3.0, 3.0)
    shifted = base + jnp.repeat(offsets, TOK_DEV, axis=0) * direction
    return jnp.clip(shifted, -10.0, 10.0).astype(jnp.bfloat16)


def gain_draw(key, salt):
    own = jax.random.fold_in(key, salt)
    base = 1.0 + 0.18 * jnp.clip(jax.random.normal(own, (HEAD,), jnp.float32), -3.0, 3.0)
    return base


def draw_query_gain(key, part):
    return gain_draw(key, 11)


def draw_key_gain(key, part):
    return gain_draw(key, 13)


def steps_of(stream_key, extent, cuts, smallest, largest):
    loudness = 1.0
    for dim, blocks in cuts:
        draws = jax.random.uniform(jax.random.fold_in(jax.random.fold_in(stream_key, 6), dim), (blocks,), jnp.float32, smallest / len(cuts), largest / len(cuts))
        loudness = loudness * jnp.repeat(jnp.exp(draws), extent[dim] // blocks).reshape((-1,) + (1,) * (len(extent) - 1 - dim))
    return loudness


def centred(stream_key, shape, spread, limit, cuts=(), held_as=jnp.bfloat16):
    factor_of = steps_of(stream_key, shape, cuts, -0.22, 0.18) if cuts else 1.0
    drawn = jax.random.normal(stream_key, shape, jnp.float32) * spread * factor_of
    return jnp.minimum(jnp.maximum(drawn, -limit), limit).astype(held_as)


def setup_inputs(seed: int = 0) -> dict:
    splits = jax.random.split(jax.random.key(seed), 8)
    tokens = draw_tokens(jax.random.fold_in(splits[7], 71), 0)
    w_query = centred(splits[1], (D, HEADS * HEAD), D ** -0.5, 0.125, ((1, 4),))
    w_key = centred(splits[2], (D, KV_HEADS * HEAD), D ** -0.5, 0.125, ((1, 4),))
    w_value = centred(splits[3], (D, KV_HEADS * HEAD), D ** -0.5, 0.125, ((1, 4),))
    w_output = centred(splits[4], (HEADS * HEAD, D), (HEADS * HEAD) ** -0.5, 0.1875, ((0, 4),))
    query_gain = draw_query_gain(jax.random.fold_in(splits[7], 71), 0)
    key_gain = draw_key_gain(jax.random.fold_in(splits[7], 71), 0)
    return dict(tokens=tokens, w_query=w_query, w_key=w_key, w_value=w_value, w_output=w_output, query_gain=query_gain, key_gain=key_gain)


ROPE_BASE = 10000.0
NORM_EPS = 1e-06

def rotate(values, position):
    dim = values.shape[-1]
    half_dim = dim // 2
    inverse = ROPE_BASE ** (-jnp.arange(half_dim, dtype=jnp.float32) * (2.0 / dim))
    angles = position.astype(jnp.float32)[:, None] * inverse[None, :]
    cosine = jnp.cos(angles)[:, None, :]
    sine = jnp.sin(angles)[:, None, :]
    first_half = values[..., :half_dim]
    second_half = values[..., half_dim:]
    return jnp.concatenate([first_half * cosine - second_half * sine, second_half * cosine + first_half * sine], -1)

def prepare(projected, gain_vec, grid_row, grid_col):
    values = projected.astype(jnp.float32)
    values = values * lax.rsqrt(lax.optimization_barrier(jnp.mean(values * values, -1, keepdims=True)) + NORM_EPS) * gain_vec
    split_at = values.shape[-1] // 2
    turned = jnp.concatenate([rotate(values[..., :split_at], grid_row), rotate(values[..., split_at:], grid_col)], -1)
    return turned.astype(jnp.bfloat16)

def reference(tokens, w_query, w_key, w_value, w_output, query_gain, key_gain):
    seq_len = tokens.shape[0]
    head_dim = query_gain.shape[0]
    query_raw = jnp.dot(tokens, w_query, preferred_element_type=jnp.float32).astype(jnp.bfloat16)
    key_raw = jnp.dot(tokens, w_key, preferred_element_type=jnp.float32).astype(jnp.bfloat16)
    value_raw = jnp.dot(tokens, w_value, preferred_element_type=jnp.float32).astype(jnp.bfloat16)
    positions = jnp.arange(seq_len, dtype=jnp.int32)
    grid_row = positions // GRID_W
    grid_col = positions % GRID_W
    queries = prepare(query_raw.reshape(seq_len, HEADS, head_dim), query_gain, grid_row, grid_col)
    key_rows = prepare(key_raw.reshape(seq_len, KV_HEADS, head_dim), key_gain, grid_row, grid_col)
    value_rows = value_raw.reshape(seq_len, KV_HEADS, head_dim).astype(jnp.float32)
    key_float = key_rows.astype(jnp.float32)
    group_size = HEADS // KV_HEADS
    block_len = math.gcd(seq_len, 256)
    n_blocks = seq_len // block_len
    query_blocks = queries.reshape(n_blocks, block_len, KV_HEADS, group_size, head_dim)
    score_scale = head_dim ** (-0.5)

    def one_block(query_block):
        scores = jnp.einsum('qkgd,skd->kgqs', query_block.astype(jnp.float32), key_float) * score_scale
        row_max = lax.optimization_barrier(jnp.max(scores, -1))
        expos = jnp.exp(scores - row_max[..., None])
        weight_sum = lax.optimization_barrier(jnp.sum(expos, -1))
        weights = expos.astype(jnp.bfloat16).astype(jnp.float32)
        summed = jnp.einsum('kgqs,skd->qkgd', weights, value_rows)
        summed = summed / jnp.transpose(weight_sum, (2, 0, 1))[..., None]
        attended_block = summed.astype(jnp.bfloat16).reshape(block_len, HEADS * head_dim)
        log_block = (row_max + jnp.log(weight_sum)).reshape(HEADS, block_len)
        return (attended_block, log_block)
    attended_all, log_all = lax.map(one_block, query_blocks)
    attended = attended_all.reshape(seq_len, HEADS * head_dim)
    log_sums = jnp.transpose(log_all, (1, 0, 2)).reshape(HEADS, seq_len)
    mixed_out = jnp.dot(attended, w_output, preferred_element_type=jnp.float32).astype(jnp.bfloat16)
    return (mixed_out, log_sums)
```

```python
import numpy as np

import jax
import jax.numpy as jnp
from jax import lax
from jax.experimental import pallas as pl
from jax.experimental.pallas import tpu as pltpu
from jax.sharding import PartitionSpec as P

GRID_W = 64
ROPE_BASE = 10000.0
NORM_EPS = 1e-06
HEAD = 64
ROWS = 192
HALF_ROWS = ROWS // 2
RING = 8
CH = RING * HALF_ROWS
PIECE = CH // 2
ST = 256
QT = 256
NQ = 4 * ROWS
NJ = 2 * NQ // QT
D = 2048
TP = 4
OUT_ROWS = ROWS // TP
LOG2E = 1.4426950408889634
LN2 = 0.6931471805599453
FLOOR = -1e30
MESH = pl.DeviceIdType.MESH
OFFSETS = (0, 1, -1, 2, -2, 3, -3, 4)
STEPS = 7
POINT = {2: 0, 3: 1, 4: 2, 5: 4, 6: 5, 7: 6, 8: 8}


def kernel(
    tok_hbm, wq_hbm, wk_hbm, wv_hbm, wo_hbm, gq_ref, gk_ref, freq_ref,
    out_ref, lse_ref,
    tok, wq, wk, wv, kv, qbuf, wo, kk0, kk1, vt0, vt1, s0, s1, mb0, mb1,
    acc_p, acc_o, m_p, m_o, acc_r, m_r, att, att_in,
    load_sem, near_send, near_recv, far_send, far_recv, q_sem, o_send, o_recv,
    att_send, att_recv, w_send, w_recv,
):
    sp = lax.axis_index("sp")
    tp = lax.axis_index("tp")
    core = lax.rem(sp, 2)
    y = lax.rem(lax.div(sp, 2), RING)
    z = lax.div(sp, 2 * RING)

    def at(z_off, y_off):
        zz = lax.rem(z + (z_off + RING), RING)
        yy = lax.rem(y + (y_off + RING), RING)
        return ((zz * RING + yy) * 2 + core, tp)

    partner = (sp + 1 - 2 * core, tp)

    def peer(d):
        return (sp, lax.rem(tp + d, TP))

    barrier = pltpu.get_barrier_semaphore()
    greeted = [at(0, o) for o in OFFSETS[1:]] + [at(o, 0) for o in OFFSETS[1:]]
    greeted += [partner] + [peer(d) for d in (1, 2, 3)]
    for device in greeted:
        pl.semaphore_signal(barrier, inc=1, device_id=device, device_id_type=MESH)

    loads = [
        pltpu.make_async_copy(src, dst, load_sem.at[n])
        for n, (src, dst) in enumerate(((tok_hbm, tok), (wk_hbm, wk), (wv_hbm, wv), (wq_hbm, wq)))
    ]
    own_w = pltpu.make_async_copy(wo_hbm, wo.at[0], load_sem.at[4])
    for load in loads:
        load.start()

    lane = lax.broadcasted_iota(jnp.int32, (16, 2 * ROWS), 1)
    token = jnp.where(lane >= ROWS, lane - ROWS, lane)
    in_row = lax.shift_right_logical(token, 6)
    grid_row = sp * (ROWS // GRID_W) + in_row
    grid_col = token - in_row * GRID_W
    freq = freq_ref[...]
    row_angle = grid_row.astype(jnp.float32) * freq
    col_angle = grid_col.astype(jnp.float32) * freq
    row_cos, row_sin = jnp.cos(row_angle), jnp.sin(row_angle)
    col_cos, col_sin = jnp.cos(col_angle), jnp.sin(col_angle)

    eye = lax.broadcasted_iota(jnp.int32, (HEAD, HEAD), 0) == lax.broadcasted_iota(
        jnp.int32, (HEAD, HEAD), 1
    )

    def column(ref):
        return jnp.sum(
            jnp.where(eye, jnp.broadcast_to(ref[...], (HEAD, HEAD)), 0.0), axis=1, keepdims=True
        )

    def prepare(u, gain, width):
        scale = lax.rsqrt(jnp.mean(u * u, axis=0, keepdims=True) + NORM_EPS)
        u = u * scale * gain
        rc, rs = row_cos[:, :width], row_sin[:, :width]
        cc, cs = col_cos[:, :width], col_sin[:, :width]
        a, b, c, d = u[0:16], u[16:32], u[32:48], u[48:64]
        return jnp.concatenate(
            [a * rc - b * rs, b * rc + a * rs, c * cc - d * cs, d * cc + c * cs], axis=0
        )

    q_gain, k_gain = column(gq_ref), column(gk_ref)

    loads[0].wait()
    loads[1].wait()
    loads[2].wait()
    x = tok[...]
    key_raw = jnp.dot(x, wk[...], preferred_element_type=jnp.float32).astype(jnp.bfloat16)
    value_raw = jnp.dot(x, wv[...], preferred_element_type=jnp.float32).astype(jnp.bfloat16)
    both_raw = jnp.concatenate([key_raw, value_raw], axis=1).astype(jnp.float32)
    turned = both_raw.T
    key_t = prepare(turned[0:HEAD], k_gain, ROWS)
    block = jnp.concatenate([key_t, turned[HEAD:]], axis=0).T.astype(jnp.bfloat16)
    kv[0, 0, 0:HALF_ROWS, :] = block[0:HALF_ROWS]
    kv[1, 0, 0:HALF_ROWS, :] = block[HALF_ROWS:]

    loads[3].wait()
    own_w.start()
    query_raw = jnp.dot(x, wq[...], preferred_element_type=jnp.float32)
    query_raw = query_raw.astype(jnp.bfloat16).astype(jnp.float32)
    pairs = jnp.concatenate([query_raw[:, 0:128], query_raw[:, 128:256]], axis=0).T

    pl.semaphore_wait(barrier, len(greeted))

    near = []
    for n in range(2):
        for u in range(1, RING):
            there = at(0, OFFSETS[u]) if n == 0 else at(OFFSETS[u], 0)
            near.append((n, u, there))
    near.sort(key=lambda item: item[1])

    def near_copy(n, u, there):
        return pltpu.make_async_remote_copy(
            src_ref=kv.at[n, 0, pl.ds(0, HALF_ROWS)],
            dst_ref=kv.at[n, 0, pl.ds(u * HALF_ROWS, HALF_ROWS)],
            send_sem=near_send.at[n, u],
            recv_sem=near_recv.at[n, u],
            device_id=there,
            device_id_type=MESH,
        )

    for item in near:
        near_copy(*item).start()

    w_rows = pl.ds(core * 128, 128)

    def w_copy(step):
        if step == 0:
            src, dst, there = wo_hbm.at[w_rows], wo.at[3, w_rows], peer(1)
        elif step == 1:
            src, dst, there = wo_hbm.at[w_rows], wo.at[1, w_rows], peer(3)
        elif step == 2:
            rows = pl.ds(core * 128, 64)
            src, dst, there = wo.at[3, rows], wo.at[2, rows], peer(1)
        elif step == 3:
            rows = pl.ds(core * 128 + 64, 64)
            src, dst, there = wo.at[1, rows], wo.at[2, rows], peer(3)
        else:
            slot = (3, 1, 2)[step - 4]
            src = dst = wo.at[slot, w_rows]
            there = partner
        return pltpu.make_async_remote_copy(
            src_ref=src,
            dst_ref=dst,
            send_sem=w_send.at[step],
            recv_sem=w_recv.at[step],
            device_id=there,
            device_id_type=MESH,
        )

    w_copy(0).start()
    w_copy(1).start()

    q_turned = jnp.concatenate(
        [prepare(pairs[0:HEAD], q_gain, 2 * ROWS), prepare(pairs[HEAD:], q_gain, 2 * ROWS)], axis=1
    ).astype(jnp.bfloat16)
    scaled = q_turned.astype(jnp.float32) * jnp.float32(LOG2E / 8.0)
    high = scaled.astype(jnp.bfloat16)
    low = (scaled - high.astype(jnp.float32)).astype(jnp.bfloat16)
    qbuf[1, 0:HEAD, :] = high
    qbuf[1, HEAD:, :] = low

    acc_p[...] = jnp.zeros_like(acc_p)
    acc_o[...] = jnp.zeros_like(acc_o)
    m_p[...] = jnp.full_like(m_p, FLOOR)
    m_o[...] = jnp.full_like(m_o, FLOOR)
    ones = lax.broadcasted_iota(jnp.int32, (16, CH), 0) == 0
    for vt in (vt0, vt1):
        vt[HEAD:, :] = jnp.where(ones, 1.0, 0.0).astype(jnp.bfloat16)

    q_copy = pltpu.make_async_remote_copy(
        src_ref=qbuf.at[1],
        dst_ref=qbuf.at[0],
        send_sem=q_sem.at[0],
        recv_sem=q_sem.at[1],
        device_id=partner,
        device_id_type=MESH,
    )
    q_copy.start()

    def far_copy(n, way, k):
        m = k // 2
        piece = k % 2
        if way == 0:
            src, dst, off = max(0, 2 * m - 1), 2 * m + 1, 1
        else:
            src, dst, off = 2 * m, min(2 * m + 2, 7), -1
            if k == STEPS - 1:
                piece = 1
        rows = pl.ds(piece * PIECE, PIECE)
        return pltpu.make_async_remote_copy(
            src_ref=kv.at[n, src, rows],
            dst_ref=kv.at[n, dst, rows],
            send_sem=far_send.at[n, way, k],
            recv_sem=far_recv.at[n, way, k],
            device_id=at(off, 0) if n == 0 else at(0, off),
            device_id_type=MESH,
        )

    def far_step(k):
        for n in range(2):
            for way in range(2):
                if k >= 2:
                    back = k - 2
                    if way == 1 and k == STEPS - 1:
                        back = k - 1
                    elif way == 1 and k == STEPS:
                        back = k - 3
                    far_copy(n, way, back).wait_recv()
                if k < STEPS:
                    far_copy(n, way, k).start()

    for k in range(2):
        for item in near:
            if item[1] // 4 == k:
                near_copy(*item).wait_recv()
        far_step(k)

    q_copy.wait_recv()

    kk = (kk0, kk1)
    vts = (vt0, vt1)
    S = (s0, s1)
    mb = (mb0, mb1)
    accs = (acc_p, acc_o)
    ms = (m_p, m_o)

    def prep(n, slot):
        blk = kv[n, slot]
        k = blk[:, :HEAD]
        kk[n][...] = jnp.concatenate([k, k], axis=1)
        vts[n][0:HEAD, :] = blk.T[HEAD:]

    def colmax(v):
        return jnp.max(v.reshape(-1, 8, QT), axis=0)

    def finish_max(buf, m):
        mb[buf][...] = jnp.broadcast_to(jnp.max(m, axis=0, keepdims=True), (8, QT))

    def cols(j):
        return slice((j % 3) * QT, (j % 3 + 1) * QT)

    def score_strip(n, j, buf, r):
        s = jnp.dot(
            kk[n][r * ST : (r + 1) * ST, :],
            qbuf[j // 3, :, cols(j)],
            preferred_element_type=jnp.float32,
        )
        S[buf][r * ST : (r + 1) * ST, :] = s
        return colmax(s)

    def scores_only(n, j, buf):
        m = None
        for r in range(CH // ST):
            v = score_strip(n, j, buf, r)
            m = v if m is None else jnp.maximum(m, v)
        finish_max(buf, m)

    def both(na, ja, ba, nb, jb, bb):
        m_ref, acc = ms[jb // 3], accs[jb // 3]
        mo = m_ref[:, cols(jb)]
        mn = jnp.maximum(mo, mb[bb][...])
        f = jnp.exp2(mo - mn)
        m = None
        ot = None
        for r in range(CH // ST):
            v = score_strip(na, ja, ba, r)
            m = v if m is None else jnp.maximum(m, v)
            strip = S[bb][r * ST : (r + 1) * ST, :].reshape(ST // 8, 8, QT)
            p = jnp.exp2(strip - mn[None]).reshape(ST, QT).astype(jnp.bfloat16)
            o = jnp.dot(vts[nb][:, r * ST : (r + 1) * ST], p, preferred_element_type=jnp.float32)
            ot = o if ot is None else ot + o
        a = acc[:, cols(jb)].reshape(10, 8, QT)
        acc[:, cols(jb)] = (a * f[None]).reshape(80, QT) + ot
        m_ref[:, cols(jb)] = mn
        finish_max(ba, m)

    prep(0, 0)
    scores_only(0, 0, 0)

    def step(i, carry):
        for n in range(2):
            for k, point in POINT.items():
                if point % 2 == n:

                    @pl.when(i == point // 2)
                    def _():
                        far_step(k)

            if n == 1:

                @pl.when(i == 5)
                def _():
                    w_copy(0).wait_recv()
                    w_copy(1).wait_recv()
                    for s in (2, 3, 4, 5):
                        w_copy(s).start()

            prep(1 - n, i if n == 0 else jnp.minimum(i + 1, RING - 1))
            for j in range(NJ):
                buf = (n * NJ + j) % 2
                if j < NJ - 1:
                    both(n, j + 1, 1 - buf, n, j, buf)
                else:
                    both(1 - n, 0, 1 - buf, n, j, buf)
        return carry

    lax.fori_loop(0, RING, step, 0)

    def o_copy(n):
        src, dst = ((acc_p, acc_r), (m_p, m_r))[n]
        return pltpu.make_async_remote_copy(
            src_ref=src,
            dst_ref=dst,
            send_sem=o_send.at[n],
            recv_sem=o_recv.at[n],
            device_id=partner,
            device_id_type=MESH,
        )

    o_copy(0).start()
    o_copy(1).start()
    w_copy(2).wait_recv()
    w_copy(3).wait_recv()
    w_copy(6).start()
    own_w.wait()
    o_copy(0).wait_recv()
    o_copy(1).wait_recv()

    m_all = jnp.maximum(m_o[...], m_r[...])
    f_o = jnp.exp2(m_o[...] - m_all)
    f_r = jnp.exp2(m_r[...] - m_all)
    total = (
        acc_o[...].reshape(10, 8, NQ) * f_o[None] + acc_r[...].reshape(10, 8, NQ) * f_r[None]
    ).reshape(80, NQ)
    weight_sum = total[HEAD : HEAD + 1]
    attended = total[0:HEAD] / weight_sum
    lse = (m_all[0:1] + jnp.log2(weight_sum)) * LN2
    for place, head in enumerate((0, 2, 1, 3)):
        lse_ref[head : head + 1, :] = lse[:, place * ROWS : (place + 1) * ROWS]
    mixed = jnp.concatenate([attended[:, : 2 * ROWS], attended[:, 2 * ROWS :]], axis=0).T
    mixed = jnp.concatenate([mixed[0:ROWS], mixed[ROWS:]], axis=1).astype(jnp.bfloat16)
    att[...] = mixed.reshape(TP, OUT_ROWS, 4 * HEAD)

    def att_copy(d):
        return pltpu.make_async_remote_copy(
            src_ref=att.at[lax.rem(tp + d, TP)],
            dst_ref=att_in.at[TP - d],
            send_sem=att_send.at[d],
            recv_sem=att_recv.at[TP - d],
            device_id=peer(d),
            device_id_type=MESH,
        )

    for d in (2, 1, 3):
        att_copy(d).start()
    result = jnp.dot(att[tp], wo[0], preferred_element_type=jnp.float32)
    for s in (4, 5, 6):
        w_copy(s).wait_recv()
    for d in (1, 3, 2):
        att_copy(TP - d).wait_recv()
        result = result + jnp.dot(att_in[d], wo[d], preferred_element_type=jnp.float32)
    out_ref[...] = result.astype(jnp.bfloat16)

    for item in near:
        near_copy(*item).wait_send()
    for n in range(2):
        for way in range(2):
            for k in range(STEPS):
                far_copy(n, way, k).wait_send()
        o_copy(n).wait_send()
    q_copy.wait_send()
    for d in (1, 2, 3):
        att_copy(d).wait_send()
    for s in range(7):
        w_copy(s).wait_send()


def shards(tokens, w_query, w_key, w_value, w_output, query_gain, key_gain):
    inverse = np.float32(ROPE_BASE) ** (-np.arange(16, dtype=np.float32) * np.float32(2.0 / 32))
    freq = jnp.asarray(np.broadcast_to(inverse.astype(np.float32)[:, None], (16, 2 * ROWS)))
    vmem = pltpu.VMEM
    bf16, f32 = jnp.bfloat16, jnp.float32
    dma = pltpu.SemaphoreType.DMA
    hbm = pl.BlockSpec(memory_space=pl.ANY)
    local = pl.BlockSpec(memory_space=vmem)
    return pl.pallas_call(
        kernel,
        out_shape=(
            jax.ShapeDtypeStruct((OUT_ROWS, D), bf16),
            jax.ShapeDtypeStruct((4, ROWS), f32),
        ),
        in_specs=[hbm] * 5 + [local] * 3,
        out_specs=(local, local),
        scratch_shapes=[
            vmem((ROWS, D), bf16),
            vmem((D, 4 * HEAD), bf16),
            vmem((D, HEAD), bf16),
            vmem((D, HEAD), bf16),
            vmem((2, RING, CH, 2 * HEAD), bf16),
            vmem((2, 2 * HEAD, NQ), bf16),
            vmem((TP, 4 * HEAD, D), bf16),
            vmem((CH, 2 * HEAD), bf16),
            vmem((CH, 2 * HEAD), bf16),
            vmem((80, CH), bf16),
            vmem((80, CH), bf16),
            vmem((CH, QT), f32),
            vmem((CH, QT), f32),
            vmem((8, QT), f32),
            vmem((8, QT), f32),
            vmem((80, NQ), f32),
            vmem((80, NQ), f32),
            vmem((8, NQ), f32),
            vmem((8, NQ), f32),
            vmem((80, NQ), f32),
            vmem((8, NQ), f32),
            vmem((TP, OUT_ROWS, 4 * HEAD), bf16),
            vmem((TP, OUT_ROWS, 4 * HEAD), bf16),
            dma((5,)),
            dma((2, RING)),
            dma((2, RING)),
            dma((2, 2, STEPS)),
            dma((2, 2, STEPS)),
            dma((2,)),
            dma((2,)),
            dma((2,)),
            dma((TP,)),
            dma((TP,)),
            dma((7,)),
            dma((7,)),
        ],
        compiler_params=pltpu.CompilerParams(
            collective_id=0, has_side_effects=True, vmem_limit_bytes=58 << 20
        ),
        name="layer",
    )(
        tokens, w_query, w_key, w_value, w_output,
        query_gain.reshape(1, HEAD), key_gain.reshape(1, HEAD), freq,
    )


def solution(mesh):
    placed = (P("sp", None), P(None, "tp"), P(None, "tp"), P(None, "tp"), P("tp", None), P(), P())
    return jax.shard_map(
        shards,
        mesh=mesh,
        in_specs=placed,
        out_specs=(P(("sp", "tp"), None), P("tp", "sp")),
        check_vma=False,
    )
```

```python
import numpy as np

import jax
import jax.numpy as jnp
from jax import lax
from jax.experimental import pallas as pl
from jax.experimental.pallas import tpu as pltpu
from jax.sharding import PartitionSpec as P

GRID_W = 64
ROPE_BASE = 10000.0
NORM_EPS = 1e-06
HEAD = 64
ROWS = 192
HALF_ROWS = ROWS // 2
RING = 8
CH_UNITS = 16
CH = CH_UNITS * HALF_ROWS
W_POINT = 16
ST = 768
QT = 256
NQ = 4 * ROWS
NJ = 2 * NQ // QT
D = 2048
TP = 4
OUT_ROWS = ROWS // TP
LOG2E = 1.4426950408889634
LN2 = 0.6931471805599453
FLOOR = -1e30
FREQUENCIES = [float(f) for f in np.float32(ROPE_BASE) ** (-np.arange(16, dtype=np.float32) * np.float32(2.0 / 32))]
MESH = pl.DeviceIdType.MESH
UNITS = 2 * RING * RING
CHUNKS = UNITS * HALF_ROWS // CH
CLASSES = ((0,), (1, -1), (2, -2), (3, -3), (4,))


def gather_plan():
    rows = (0, 1, -1, 2, -2, 3, -3, 4)
    order = []
    for row in rows:
        for c, offsets in enumerate(CLASSES):
            for n in range(2):
                order.append((abs(row) + (c > 0), c, n, rows.index(row), offsets))
    order.sort()
    slot = {}
    for _, _, n, r, offsets in order:
        for o in offsets:
            slot[n, rows[r], o] = len(slot)
    copies = []
    for n in range(2):
        for c in range(1, len(CLASSES)):
            for o in CLASSES[c]:
                copies.append(((0, 0), (1, c), (n, 0, 0), (n, 0, o), 1, n, True, o))
        for c, offsets in enumerate(CLASSES):
            for way in (1, -1):
                for step in range(4):
                    row, to = way * step, way * (step + 1)
                    part = offsets
                    if step == 3:
                        to = 4
                        if len(offsets) == 2:
                            part = offsets[:1] if way == 1 else offsets[1:]
                        elif (way == 1) != ((n == 0) == (c == 0)):
                            part = ()
                    if part:
                        copies.append(
                            ((step + (c > 0), c), (step + 1 + (c > 0), c), (n, row, part[0]), (n, to, part[0]), len(part), n, False, way)
                        )
    copies.sort(key=lambda copy: (copy[0], copy[6]))
    return slot, copies


SLOT, COPIES = gather_plan()
GROUPS = sorted({copy[1] for copy in COPIES})
POINT = {
    (1, 0): -1, (1, 1): -1, (1, 2): -1, (1, 3): -1, (1, 4): 2, (2, 0): 2, (2, 1): 2, (2, 2): 3, (2, 3): 5, (2, 4): 6, (3, 0): 6, (3, 1): 7, (3, 2): 8, (3, 3): 10, (3, 4): 11, (4, 0): 11, (4, 1): 12, (4, 2): 13, (4, 3): 14, (4, 4): 15, (5, 1): 16, (5, 2): 17, (5, 3): 18, (5, 4): 19,
}
THIRDS = (0, 2, 4)


def kernel(
    tok_hbm, wq_hbm, wk_hbm, wv_hbm, wo_hbm, gq_ref, gk_ref,
    out_ref, lse_ref,
    tok, wq, wk, wv, kv, qbuf, wo, kk0, kk1, vt0, vt1, s0, s1, mb0, mb1,
    acc_p, acc_o, m_p, m_o, acc_r, m_r, att, att_in,
    load_sem, kv_send, kv_recv, q_sem, o_send, o_recv,
    att_send, att_recv, w_send, w_recv,
):
    sp = lax.axis_index("sp")
    tp = lax.axis_index("tp")
    core = lax.rem(sp, 2)
    y = lax.rem(lax.div(sp, 2), RING)
    z = lax.div(sp, 2 * RING)

    def at(z_off, y_off):
        zz = lax.rem(z + (z_off + RING), RING)
        yy = lax.rem(y + (y_off + RING), RING)
        return ((zz * RING + yy) * 2 + core, tp)

    partner = (sp + 1 - 2 * core, tp)

    def peer(d):
        return (sp, lax.rem(tp + d, TP))

    barrier = pltpu.get_barrier_semaphore()
    greeted = [at(0, o) for c in CLASSES[1:] for o in c] + [at(o, 0) for c in CLASSES[1:] for o in c]
    greeted += [partner] + [peer(d) for d in (1, 2, 3)]
    for device in greeted:
        pl.semaphore_signal(barrier, inc=1, device_id=device, device_id_type=MESH)

    loads = [
        pltpu.make_async_copy(src, dst, load_sem.at[n])
        for n, (src, dst) in enumerate(((tok_hbm, tok), (wk_hbm, wk), (wv_hbm, wv), (wq_hbm, wq)))
    ]
    own_w = pltpu.make_async_copy(wo_hbm, wo.at[0], load_sem.at[4])
    for load in loads:
        load.start()

    lane = lax.broadcasted_iota(jnp.int32, (16, 2 * ROWS), 1)
    token = jnp.where(lane >= ROWS, lane - ROWS, lane)
    in_row = lax.shift_right_logical(token, 6)
    grid_row = sp * (ROWS // GRID_W) + in_row
    grid_col = token - in_row * GRID_W
    channel = lax.broadcasted_iota(jnp.int32, (16, 128), 0)
    freq = jnp.zeros((16, 128), jnp.float32)
    for n in range(16):
        freq = jnp.where(channel == n, FREQUENCIES[n], freq)
    freq = jnp.concatenate([freq, freq, freq], axis=1)
    row_angle = grid_row.astype(jnp.float32) * freq
    col_angle = grid_col.astype(jnp.float32) * freq
    row_cos, row_sin = jnp.cos(row_angle), jnp.sin(row_angle)
    col_cos, col_sin = jnp.cos(col_angle), jnp.sin(col_angle)

    eye = lax.broadcasted_iota(jnp.int32, (HEAD, HEAD), 0) == lax.broadcasted_iota(
        jnp.int32, (HEAD, HEAD), 1
    )

    def column(ref):
        return jnp.sum(
            jnp.where(eye, jnp.broadcast_to(ref[...], (HEAD, HEAD)), 0.0), axis=1, keepdims=True
        )

    def prepare(u, gain, width):
        scale = lax.rsqrt(jnp.mean(u * u, axis=0, keepdims=True) + NORM_EPS)
        u = u * scale * gain
        rc, rs = row_cos[:, :width], row_sin[:, :width]
        cc, cs = col_cos[:, :width], col_sin[:, :width]
        a, b, c, d = u[0:16], u[16:32], u[32:48], u[48:64]
        return jnp.concatenate(
            [a * rc - b * rs, b * rc + a * rs, c * cc - d * cs, d * cc + c * cs], axis=0
        )

    q_gain, k_gain = column(gq_ref), column(gk_ref)

    def project(w, x):
        return lax.dot_general(w, x, (((1,), (1,)), ((), ())), preferred_element_type=jnp.float32)


    loads[0].wait()
    loads[1].wait()
    loads[2].wait()
    x = tok[...]
    key_raw = project(wk[...], x).astype(jnp.bfloat16).astype(jnp.float32)
    value_raw = project(wv[...], x).astype(jnp.bfloat16).astype(jnp.float32)
    key_t = prepare(key_raw, k_gain, ROWS)
    block = jnp.concatenate([key_t, value_raw], axis=0).T.astype(jnp.bfloat16)
    kv[SLOT[0, 0, 0]] = block[0:HALF_ROWS]
    kv[SLOT[1, 0, 0]] = block[HALF_ROWS:]

    pl.semaphore_wait(barrier, len(greeted))

    def kv_copy(m):
        _, _, source, target, units, n, near, places = COPIES[m]
        along_y = (n == 0) == near
        return pltpu.make_async_remote_copy(
            src_ref=kv.at[pl.ds(SLOT[source], units)],
            dst_ref=kv.at[pl.ds(SLOT[target], units)],
            send_sem=kv_send.at[m],
            recv_sem=kv_recv.at[m],
            device_id=at(0, places) if along_y else at(places, 0),
            device_id_type=MESH,
        )

    def forward(group):
        for m, copy in enumerate(COPIES):
            if copy[1] == group:
                kv_copy(m).wait_recv()
        for m, copy in enumerate(COPIES):
            if copy[0] == group:
                kv_copy(m).start()

    forward((0, 0))

    loads[3].wait()
    own_w.start()
    query_raw = jnp.dot(x, wq[...], preferred_element_type=jnp.float32)
    query_raw = query_raw.astype(jnp.bfloat16).astype(jnp.float32)
    pairs = jnp.concatenate([query_raw[:, 0:128], query_raw[:, 128:256]], axis=0).T

    w_rows = pl.ds(core * 128, 128)

    def w_copy(step):
        if step == 0:
            src, dst, there = wo_hbm.at[w_rows], wo.at[3, w_rows], peer(1)
        elif step == 1:
            src, dst, there = wo_hbm.at[w_rows], wo.at[1, w_rows], peer(3)
        elif step == 2:
            rows = pl.ds(core * 128, 64)
            src, dst, there = wo.at[3, rows], wo.at[2, rows], peer(1)
        elif step == 3:
            rows = pl.ds(core * 128 + 64, 64)
            src, dst, there = wo.at[1, rows], wo.at[2, rows], peer(3)
        else:
            slot = (3, 1, 2)[step - 4]
            src = dst = wo.at[slot, w_rows]
            there = partner
        return pltpu.make_async_remote_copy(
            src_ref=src,
            dst_ref=dst,
            send_sem=w_send.at[step],
            recv_sem=w_recv.at[step],
            device_id=there,
            device_id_type=MESH,
        )

    w_copy(0).start()
    w_copy(1).start()

    q_turned = jnp.concatenate(
        [prepare(pairs[0:HEAD], q_gain, 2 * ROWS), prepare(pairs[HEAD:], q_gain, 2 * ROWS)], axis=1
    ).astype(jnp.bfloat16)
    scaled = q_turned.astype(jnp.float32) * jnp.float32(LOG2E / 8.0)
    high = scaled.astype(jnp.bfloat16)
    low = (scaled - high.astype(jnp.float32)).astype(jnp.bfloat16)
    qbuf[1, 0:HEAD, :] = high
    qbuf[1, HEAD:, :] = low

    acc_p[...] = jnp.zeros_like(acc_p)
    acc_o[...] = jnp.zeros_like(acc_o)
    m_p[...] = jnp.full_like(m_p, FLOOR)
    m_o[...] = jnp.full_like(m_o, FLOOR)
    ones = lax.broadcasted_iota(jnp.int32, (16, CH), 0) == 0
    for vt in (vt0, vt1):
        vt[HEAD:, :] = jnp.where(ones, 1.0, 0.0).astype(jnp.bfloat16)

    q_copy = pltpu.make_async_remote_copy(
        src_ref=qbuf.at[1],
        dst_ref=qbuf.at[0],
        send_sem=q_sem.at[0],
        recv_sem=q_sem.at[1],
        device_id=partner,
        device_id_type=MESH,
    )
    q_copy.start()

    for group in GROUPS:
        if POINT[group] < 0:
            forward(group)

    q_copy.wait_recv()

    kk = (kk0, kk1)
    vts = (vt0, vt1)
    S = (s0, s1)
    mb = (mb0, mb1)
    accs = (acc_p, acc_o)
    ms = (m_p, m_o)

    def prep(n, c):
        blk = kv[pl.ds(pl.multiple_of(c * CH_UNITS, CH_UNITS), CH_UNITS)].reshape(CH, 2 * HEAD)
        k = blk[:, :HEAD]
        kk[n][...] = jnp.concatenate([k, k], axis=1)
        vts[n][0:HEAD, :] = blk.T[HEAD:]

    def colmax(v):
        return jnp.max(v.reshape(-1, 8, QT), axis=0)

    def finish_max(buf, m):
        mb[buf][...] = jnp.broadcast_to(jnp.max(m, axis=0, keepdims=True), (8, QT))

    def cols(j):
        return slice((j % 3) * QT, (j % 3 + 1) * QT)

    def score_strip(n, j, buf, r):
        s = jnp.dot(
            kk[n][r * ST : (r + 1) * ST, :],
            qbuf[j // 3, :, cols(j)],
            preferred_element_type=jnp.float32,
        )
        S[buf][r * ST : (r + 1) * ST, :] = s
        return colmax(s)

    def scores_only(n, j, buf):
        m = None
        for r in range(CH // ST):
            v = score_strip(n, j, buf, r)
            m = v if m is None else jnp.maximum(m, v)
        finish_max(buf, m)

    def both(na, ja, ba, nb, jb, bb):
        m_ref, acc = ms[jb // 3], accs[jb // 3]
        mo = m_ref[:, cols(jb)]
        mn = jnp.maximum(mo, mb[bb][...])
        f = jnp.exp2(mo - mn)
        m = None
        ot = None
        for r in range(CH // ST):
            v = score_strip(na, ja, ba, r)
            m = v if m is None else jnp.maximum(m, v)
            strip = S[bb][r * ST : (r + 1) * ST, :].reshape(ST // 8, 8, QT)
            p = jnp.exp2(strip - mn[None]).reshape(ST, QT).astype(jnp.bfloat16)
            o = jnp.dot(vts[nb][:, r * ST : (r + 1) * ST], p, preferred_element_type=jnp.float32)
            ot = o if ot is None else ot + o
        a = acc[:, cols(jb)].reshape(10, 8, QT)
        acc[:, cols(jb)] = (a * f[None]).reshape(80, QT) + ot
        m_ref[:, cols(jb)] = mn
        finish_max(ba, m)

    def o_copy(n):
        src, dst = ((acc_p, acc_r), (m_p, m_r))[n]
        return pltpu.make_async_remote_copy(
            src_ref=src,
            dst_ref=dst,
            send_sem=o_send.at[n],
            recv_sem=o_recv.at[n],
            device_id=partner,
            device_id_type=MESH,
        )

    prep(0, 0)
    scores_only(0, 0, 0)

    def step(i, carry):
        for n in range(2):
            for j in range(NJ):
                buf = (n * NJ + j) % 2
                if j in THIRDS:
                    third = THIRDS.index(j)
                    for group in GROUPS:
                        if POINT[group] >= 0 and POINT[group] % 6 == 3 * n + third:

                            @pl.when(i == POINT[group] // 6)
                            def _():
                                forward(group)

                    if W_POINT % 6 == 3 * n + third:

                        @pl.when(i == W_POINT // 6)
                        def _():
                            w_copy(0).wait_recv()
                            w_copy(1).wait_recv()
                            for s in (2, 3, 4, 5):
                                w_copy(s).start()

                    if n == 1 and third == 2:

                        @pl.when(i == CHUNKS // 2 - 1)
                        def _():
                            o_copy(0).start()
                            o_copy(1).start()

                    if third == 2:
                        prep(1 - n, jnp.minimum(2 * i + n + 1, CHUNKS - 1))
                if j < NJ - 1:
                    both(n, j + 1, 1 - buf, n, j, buf)
                else:
                    both(1 - n, 0, 1 - buf, n, j, buf)
        return carry

    lax.fori_loop(0, CHUNKS // 2, step, 0)

    w_copy(2).wait_recv()
    w_copy(3).wait_recv()
    w_copy(6).start()
    own_w.wait()
    o_copy(0).wait_recv()
    o_copy(1).wait_recv()

    m_all = jnp.maximum(m_o[...], m_r[...])
    f_o = jnp.exp2(m_o[...] - m_all)
    f_r = jnp.exp2(m_r[...] - m_all)
    total = (
        acc_o[...].reshape(10, 8, NQ) * f_o[None] + acc_r[...].reshape(10, 8, NQ) * f_r[None]
    ).reshape(80, NQ)
    weight_sum = total[HEAD : HEAD + 1]
    attended = total[0:HEAD] / weight_sum
    lse = (m_all[0:1] + jnp.log2(weight_sum)) * LN2
    for place, head in enumerate((0, 2, 1, 3)):
        lse_ref[head : head + 1, :] = lse[:, place * ROWS : (place + 1) * ROWS]
    mixed = jnp.concatenate([attended[:, : 2 * ROWS], attended[:, 2 * ROWS :]], axis=0).T
    mixed = jnp.concatenate([mixed[0:ROWS], mixed[ROWS:]], axis=1).astype(jnp.bfloat16)
    att[...] = mixed.reshape(TP, OUT_ROWS, 4 * HEAD)

    def att_copy(d):
        return pltpu.make_async_remote_copy(
            src_ref=att.at[lax.rem(tp + d, TP)],
            dst_ref=att_in.at[TP - d],
            send_sem=att_send.at[d],
            recv_sem=att_recv.at[TP - d],
            device_id=peer(d),
            device_id_type=MESH,
        )

    for d in (2, 1, 3):
        att_copy(d).start()
    result = jnp.dot(att[tp], wo[0], preferred_element_type=jnp.float32)
    for s in (4, 5, 6):
        w_copy(s).wait_recv()
    for d in (1, 3, 2):
        att_copy(TP - d).wait_recv()
        result = result + jnp.dot(att_in[d], wo[d], preferred_element_type=jnp.float32)
    out_ref[...] = result.astype(jnp.bfloat16)

    for m in range(len(COPIES)):
        kv_copy(m).wait_send()
    for n in range(2):
        o_copy(n).wait_send()
    q_copy.wait_send()
    for d in (1, 2, 3):
        att_copy(d).wait_send()
    for s in range(7):
        w_copy(s).wait_send()


def shards(tokens, w_query, w_key, w_value, w_output, query_gain, key_gain):
    vmem = pltpu.VMEM
    bf16, f32 = jnp.bfloat16, jnp.float32
    dma = pltpu.SemaphoreType.DMA
    hbm = pl.BlockSpec(memory_space=pl.ANY)
    local = pl.BlockSpec(memory_space=vmem)
    return pl.pallas_call(
        kernel,
        out_shape=(
            jax.ShapeDtypeStruct((OUT_ROWS, D), bf16),
            jax.ShapeDtypeStruct((4, ROWS), f32),
        ),
        in_specs=[hbm] * 5 + [local] * 2,
        out_specs=(local, local),
        scratch_shapes=[
            vmem((ROWS, D), bf16),
            vmem((D, 4 * HEAD), bf16),
            vmem((HEAD, D), bf16),
            vmem((HEAD, D), bf16),
            vmem((UNITS, HALF_ROWS, 2 * HEAD), bf16),
            vmem((2, 2 * HEAD, NQ), bf16),
            vmem((TP, 4 * HEAD, D), bf16),
            vmem((CH, 2 * HEAD), bf16),
            vmem((CH, 2 * HEAD), bf16),
            vmem((80, CH), bf16),
            vmem((80, CH), bf16),
            vmem((CH, QT), f32),
            vmem((CH, QT), f32),
            vmem((8, QT), f32),
            vmem((8, QT), f32),
            vmem((80, NQ), f32),
            vmem((80, NQ), f32),
            vmem((8, NQ), f32),
            vmem((8, NQ), f32),
            vmem((80, NQ), f32),
            vmem((8, NQ), f32),
            vmem((TP, OUT_ROWS, 4 * HEAD), bf16),
            vmem((TP, OUT_ROWS, 4 * HEAD), bf16),
            dma((5,)),
            dma((len(COPIES),)),
            dma((len(COPIES),)),
            dma((2,)),
            dma((2,)),
            dma((2,)),
            dma((TP,)),
            dma((TP,)),
            dma((7,)),
            dma((7,)),
        ],
        compiler_params=pltpu.CompilerParams(
            collective_id=0, has_side_effects=True, vmem_limit_bytes=58 << 20
        ),
        name="layer",
    )(
        tokens, w_query, w_key.T, w_value.T, w_output,
        query_gain.reshape(1, HEAD), key_gain.reshape(1, HEAD),
    )


def solution(mesh):
    placed = (P("sp", None), P(None, "tp"), P(None, "tp"), P(None, "tp"), P("tp", None), P(), P())
    return jax.shard_map(
        shards,
        mesh=mesh,
        in_specs=placed,
        out_specs=(P(("sp", "tp"), None), P("tp", "sp")),
        check_vma=False,
    )
```

```python
import numpy as np

import jax
import jax.numpy as jnp
from jax import lax
from jax.experimental import pallas as pl
from jax.experimental.pallas import tpu as pltpu
from jax.sharding import PartitionSpec as P

GRID_W = 64
ROPE_BASE = 10000.0
NORM_EPS = 1e-06
HEAD = 64
ROWS = 192
HALF_ROWS = ROWS // 2
RING = 8
CH_UNITS = 16
CH = CH_UNITS * HALF_ROWS
W_POINT = 16
ST = 768
QT = 256
NQ = 4 * ROWS
NJ = 2 * NQ // QT
D = 2048
TP = 4
OUT_ROWS = ROWS // TP
LOG2E = 1.4426950408889634
LN2 = 0.6931471805599453
FLOOR = -1e30
FREQUENCIES = [float(f) for f in np.float32(ROPE_BASE) ** (-np.arange(16, dtype=np.float32) * np.float32(2.0 / 32))]
MESH = pl.DeviceIdType.MESH
UNITS = 2 * RING * RING
CHUNKS = UNITS * HALF_ROWS // CH
CLASSES = ((0,), (1, -1), (2, -2), (3, -3), (4,))


def gather_plan():
    rows = (0, 1, -1, 2, -2, 3, -3, 4)
    order = []
    for row in rows:
        for c, offsets in enumerate(CLASSES):
            for n in range(2):
                order.append((abs(row) + (c > 0), c, n, rows.index(row), offsets))
    order.sort()
    slot = {}
    for _, _, n, r, offsets in order:
        for o in offsets:
            slot[n, rows[r], o] = len(slot)
    copies = []
    for n in range(2):
        for c in range(1, len(CLASSES)):
            for o in CLASSES[c]:
                copies.append(((0, 0), (1, c), (n, 0, 0), (n, 0, o), 1, n, True, o))
        for c, offsets in enumerate(CLASSES):
            for way in (1, -1):
                for step in range(4):
                    row, to = way * step, way * (step + 1)
                    part = offsets
                    if step == 3:
                        to = 4
                        if len(offsets) == 2:
                            part = offsets[:1] if way == 1 else offsets[1:]
                        elif (way == 1) != ((n == 0) == (c == 0)):
                            part = ()
                    if part:
                        copies.append(
                            ((step + (c > 0), c), (step + 1 + (c > 0), c), (n, row, part[0]), (n, to, part[0]), len(part), n, False, way)
                        )
    copies.sort(key=lambda copy: (copy[0], copy[6]))
    return slot, copies


SLOT, COPIES = gather_plan()
GROUPS = sorted({copy[1] for copy in COPIES})
POINT = {
    (1, 0): -1, (1, 1): -1, (1, 2): -1, (1, 3): -1, (1, 4): 2, (2, 0): 2, (2, 1): 2, (2, 2): 4, (2, 3): 5, (2, 4): 6, (3, 0): 6, (3, 1): 8, (3, 2): 9, (3, 3): 11, (3, 4): 12, (4, 0): 12, (4, 1): 13, (4, 2): 14, (4, 3): 15, (4, 4): 16, (5, 1): 17, (5, 2): 18, (5, 3): 19, (5, 4): 20,
}
THIRDS = (0, 2, 4)


def kernel(
    tok_hbm, wq_hbm, wk_hbm, wv_hbm, wo_hbm, gq_ref, gk_ref,
    out_ref, lse_ref,
    tok, wq, wk, wv, kv, qbuf, wo, kk0, kk1, vt0, vt1, s0, s1, mb0, mb1,
    acc_p, acc_o, m_p, m_o, acc_r, m_r, att, att_in,
    load_sem, kv_send, kv_recv, q_sem, o_send, o_recv,
    att_send, att_recv, w_send, w_recv,
):
    sp = lax.axis_index("sp")
    tp = lax.axis_index("tp")
    core = lax.rem(sp, 2)
    y = lax.rem(lax.div(sp, 2), RING)
    z = lax.div(sp, 2 * RING)

    def at(z_off, y_off):
        zz = lax.rem(z + (z_off + RING), RING)
        yy = lax.rem(y + (y_off + RING), RING)
        return ((zz * RING + yy) * 2 + core, tp)

    partner = (sp + 1 - 2 * core, tp)

    def peer(d):
        return (sp, lax.rem(tp + d, TP))

    barrier = pltpu.get_barrier_semaphore()
    greeted = [at(0, o) for c in CLASSES[1:] for o in c] + [at(o, 0) for c in CLASSES[1:] for o in c]
    greeted += [partner] + [peer(d) for d in (1, 2, 3)]
    for device in greeted:
        pl.semaphore_signal(barrier, inc=1, device_id=device, device_id_type=MESH)

    loads = [
        pltpu.make_async_copy(src, dst, load_sem.at[n])
        for n, (src, dst) in enumerate(((tok_hbm, tok), (wk_hbm, wk), (wv_hbm, wv), (wq_hbm, wq)))
    ]
    own_w = pltpu.make_async_copy(wo_hbm, wo.at[0], load_sem.at[4])
    for load in loads:
        load.start()

    lane = lax.broadcasted_iota(jnp.int32, (16, 2 * ROWS), 1)
    token = jnp.where(lane >= ROWS, lane - ROWS, lane)
    in_row = lax.shift_right_logical(token, 6)
    grid_row = sp * (ROWS // GRID_W) + in_row
    grid_col = token - in_row * GRID_W
    channel = lax.broadcasted_iota(jnp.int32, (16, 128), 0)
    freq = jnp.zeros((16, 128), jnp.float32)
    for n in range(16):
        freq = jnp.where(channel == n, FREQUENCIES[n], freq)
    freq = jnp.concatenate([freq, freq, freq], axis=1)
    row_angle = grid_row.astype(jnp.float32) * freq
    col_angle = grid_col.astype(jnp.float32) * freq
    row_cos, row_sin = jnp.cos(row_angle), jnp.sin(row_angle)
    col_cos, col_sin = jnp.cos(col_angle), jnp.sin(col_angle)

    eye = lax.broadcasted_iota(jnp.int32, (HEAD, HEAD), 0) == lax.broadcasted_iota(
        jnp.int32, (HEAD, HEAD), 1
    )

    def column(ref):
        return jnp.sum(
            jnp.where(eye, jnp.broadcast_to(ref[...], (HEAD, HEAD)), 0.0), axis=1, keepdims=True
        )

    def prepare(u, gain, width):
        scale = lax.rsqrt(jnp.mean(u * u, axis=0, keepdims=True) + NORM_EPS)
        u = u * scale * gain
        rc, rs = row_cos[:, :width], row_sin[:, :width]
        cc, cs = col_cos[:, :width], col_sin[:, :width]
        a, b, c, d = u[0:16], u[16:32], u[32:48], u[48:64]
        return jnp.concatenate(
            [a * rc - b * rs, b * rc + a * rs, c * cc - d * cs, d * cc + c * cs], axis=0
        )

    q_gain, k_gain = column(gq_ref), column(gk_ref)

    def project(w, x):
        return lax.dot_general(w, x, (((1,), (1,)), ((), ())), preferred_element_type=jnp.float32)


    loads[0].wait()
    loads[1].wait()
    loads[2].wait()
    x = tok[...]
    key_raw = project(wk[...], x).astype(jnp.bfloat16).astype(jnp.float32)
    value_raw = project(wv[...], x).astype(jnp.bfloat16).astype(jnp.float32)
    key_t = prepare(key_raw, k_gain, ROWS)
    block = jnp.concatenate([key_t, value_raw], axis=0).T.astype(jnp.bfloat16)
    kv[SLOT[0, 0, 0]] = block[0:HALF_ROWS]
    kv[SLOT[1, 0, 0]] = block[HALF_ROWS:]

    pl.semaphore_wait(barrier, len(greeted))

    def kv_copy(m):
        _, _, source, target, units, n, near, places = COPIES[m]
        along_y = (n == 0) == near
        return pltpu.make_async_remote_copy(
            src_ref=kv.at[pl.ds(SLOT[source], units)],
            dst_ref=kv.at[pl.ds(SLOT[target], units)],
            send_sem=kv_send.at[m],
            recv_sem=kv_recv.at[m],
            device_id=at(0, places) if along_y else at(places, 0),
            device_id_type=MESH,
        )

    def forward(group):
        for m, copy in enumerate(COPIES):
            if copy[1] == group:
                kv_copy(m).wait_recv()
        for m, copy in enumerate(COPIES):
            if copy[0] == group:
                kv_copy(m).start()

    forward((0, 0))

    loads[3].wait()
    own_w.start()
    query_raw = jnp.dot(x, wq[...], preferred_element_type=jnp.float32)
    query_raw = query_raw.astype(jnp.bfloat16).astype(jnp.float32)
    pairs = jnp.concatenate([query_raw[:, 0:128], query_raw[:, 128:256]], axis=0).T

    w_rows = pl.ds(core * 128, 128)

    def w_copy(step):
        if step == 0:
            src, dst, there = wo_hbm.at[w_rows], wo.at[3, w_rows], peer(1)
        elif step == 1:
            src, dst, there = wo_hbm.at[w_rows], wo.at[1, w_rows], peer(3)
        elif step == 2:
            rows = pl.ds(core * 128, 64)
            src, dst, there = wo.at[3, rows], wo.at[2, rows], peer(1)
        elif step == 3:
            rows = pl.ds(core * 128 + 64, 64)
            src, dst, there = wo.at[1, rows], wo.at[2, rows], peer(3)
        else:
            slot = (3, 1, 2)[step - 4]
            src = dst = wo.at[slot, w_rows]
            there = partner
        return pltpu.make_async_remote_copy(
            src_ref=src,
            dst_ref=dst,
            send_sem=w_send.at[step],
            recv_sem=w_recv.at[step],
            device_id=there,
            device_id_type=MESH,
        )

    w_copy(0).start()
    w_copy(1).start()

    q_turned = jnp.concatenate(
        [prepare(pairs[0:HEAD], q_gain, 2 * ROWS), prepare(pairs[HEAD:], q_gain, 2 * ROWS)], axis=1
    ).astype(jnp.bfloat16)
    scaled = q_turned.astype(jnp.float32) * jnp.float32(LOG2E / 8.0)
    high = scaled.astype(jnp.bfloat16)
    low = (scaled - high.astype(jnp.float32)).astype(jnp.bfloat16)
    qbuf[1, 0:HEAD, :] = high
    qbuf[1, HEAD:, :] = low

    acc_p[...] = jnp.zeros_like(acc_p)
    acc_o[...] = jnp.zeros_like(acc_o)
    m_p[...] = jnp.full_like(m_p, FLOOR)
    m_o[...] = jnp.full_like(m_o, FLOOR)
    ones = lax.broadcasted_iota(jnp.int32, (16, CH), 0) == 0
    for vt in (vt0, vt1):
        vt[HEAD:, :] = jnp.where(ones, 1.0, 0.0).astype(jnp.bfloat16)

    q_copy = pltpu.make_async_remote_copy(
        src_ref=qbuf.at[1],
        dst_ref=qbuf.at[0],
        send_sem=q_sem.at[0],
        recv_sem=q_sem.at[1],
        device_id=partner,
        device_id_type=MESH,
    )
    q_copy.start()

    for group in GROUPS:
        if POINT[group] < 0:
            forward(group)

    q_copy.wait_recv()

    kk = (kk0, kk1)
    vts = (vt0, vt1)
    S = (s0, s1)
    mb = (mb0, mb1)
    accs = (acc_p, acc_o)
    ms = (m_p, m_o)

    def prep(n, c):
        blk = kv[pl.ds(pl.multiple_of(c * CH_UNITS, CH_UNITS), CH_UNITS)].reshape(CH, 2 * HEAD)
        k = blk[:, :HEAD]
        kk[n][...] = jnp.concatenate([k, k], axis=1)
        vts[n][0:HEAD, :] = blk.T[HEAD:]

    def colmax(v):
        return jnp.max(v.reshape(-1, 8, QT), axis=0)

    def finish_max(buf, m):
        mb[buf][...] = jnp.broadcast_to(jnp.max(m, axis=0, keepdims=True), (8, QT))

    def cols(j):
        return slice((j % 3) * QT, (j % 3 + 1) * QT)

    def score_strip(n, j, buf, r):
        s = jnp.dot(
            kk[n][r * ST : (r + 1) * ST, :],
            qbuf[j // 3, :, cols(j)],
            preferred_element_type=jnp.float32,
        )
        S[buf][r * ST : (r + 1) * ST, :] = s
        return colmax(s)

    def scores_only(n, j, buf):
        m = None
        for r in range(CH // ST):
            v = score_strip(n, j, buf, r)
            m = v if m is None else jnp.maximum(m, v)
        finish_max(buf, m)

    def both(na, ja, ba, nb, jb, bb):
        m_ref, acc = ms[jb // 3], accs[jb // 3]
        mo = m_ref[:, cols(jb)]
        mn = jnp.maximum(mo, mb[bb][...])
        f = jnp.exp2(mo - mn)
        m = None
        ot = None
        for r in range(CH // ST):
            v = score_strip(na, ja, ba, r)
            m = v if m is None else jnp.maximum(m, v)
            strip = S[bb][r * ST : (r + 1) * ST, :].reshape(ST // 8, 8, QT)
            p = jnp.exp2(strip - mn[None]).reshape(ST, QT).astype(jnp.bfloat16)
            o = jnp.dot(vts[nb][:, r * ST : (r + 1) * ST], p, preferred_element_type=jnp.float32)
            ot = o if ot is None else ot + o
        a = acc[:, cols(jb)].reshape(10, 8, QT)
        acc[:, cols(jb)] = (a * f[None]).reshape(80, QT) + ot
        m_ref[:, cols(jb)] = mn
        finish_max(ba, m)

    def o_copy(n):
        src, dst = ((acc_p, acc_r), (m_p, m_r))[n]
        return pltpu.make_async_remote_copy(
            src_ref=src,
            dst_ref=dst,
            send_sem=o_send.at[n],
            recv_sem=o_recv.at[n],
            device_id=partner,
            device_id_type=MESH,
        )

    prep(0, 0)
    scores_only(0, 0, 0)

    def step(i, carry):
        for n in range(2):
            for j in range(NJ):
                buf = (n * NJ + j) % 2
                if j in THIRDS:
                    third = THIRDS.index(j)
                    for group in GROUPS:
                        if POINT[group] >= 0 and POINT[group] % 6 == 3 * n + third:

                            @pl.when(i == POINT[group] // 6)
                            def _():
                                forward(group)

                    if W_POINT % 6 == 3 * n + third:

                        @pl.when(i == W_POINT // 6)
                        def _():
                            w_copy(0).wait_recv()
                            w_copy(1).wait_recv()
                            for s in (2, 3, 4, 5):
                                w_copy(s).start()

                    if n == 1 and third == 2:

                        @pl.when(i == CHUNKS // 2 - 1)
                        def _():
                            o_copy(0).start()
                            o_copy(1).start()

                    if third == 2:
                        prep(1 - n, jnp.minimum(2 * i + n + 1, CHUNKS - 1))
                if j < NJ - 1:
                    both(n, j + 1, 1 - buf, n, j, buf)
                else:
                    both(1 - n, 0, 1 - buf, n, j, buf)
        return carry

    lax.fori_loop(0, CHUNKS // 2, step, 0)

    w_copy(2).wait_recv()
    w_copy(3).wait_recv()
    w_copy(6).start()
    own_w.wait()
    o_copy(0).wait_recv()
    o_copy(1).wait_recv()

    m_all = jnp.maximum(m_o[...], m_r[...])
    f_o = jnp.exp2(m_o[...] - m_all)
    f_r = jnp.exp2(m_r[...] - m_all)
    total = (
        acc_o[...].reshape(10, 8, NQ) * f_o[None] + acc_r[...].reshape(10, 8, NQ) * f_r[None]
    ).reshape(80, NQ)
    weight_sum = total[HEAD : HEAD + 1]
    attended = total[0:HEAD] / weight_sum
    lse = (m_all[0:1] + jnp.log2(weight_sum)) * LN2
    for place, head in enumerate((0, 2, 1, 3)):
        lse_ref[head : head + 1, :] = lse[:, place * ROWS : (place + 1) * ROWS]
    mixed = jnp.concatenate([attended[:, : 2 * ROWS], attended[:, 2 * ROWS :]], axis=0).T
    mixed = jnp.concatenate([mixed[0:ROWS], mixed[ROWS:]], axis=1).astype(jnp.bfloat16)
    att[...] = mixed.reshape(TP, OUT_ROWS, 4 * HEAD)

    def att_copy(d):
        return pltpu.make_async_remote_copy(
            src_ref=att.at[lax.rem(tp + d, TP)],
            dst_ref=att_in.at[TP - d],
            send_sem=att_send.at[d],
            recv_sem=att_recv.at[TP - d],
            device_id=peer(d),
            device_id_type=MESH,
        )

    for d in (2, 1, 3):
        att_copy(d).start()
    result = jnp.dot(att[tp], wo[0], preferred_element_type=jnp.float32)
    for s in (4, 5, 6):
        w_copy(s).wait_recv()
    for d in (1, 3, 2):
        att_copy(TP - d).wait_recv()
        result = result + jnp.dot(att_in[d], wo[d], preferred_element_type=jnp.float32)
    out_ref[...] = result.astype(jnp.bfloat16)

    for m in range(len(COPIES)):
        kv_copy(m).wait_send()
    for n in range(2):
        o_copy(n).wait_send()
    q_copy.wait_send()
    for d in (1, 2, 3):
        att_copy(d).wait_send()
    for s in range(7):
        w_copy(s).wait_send()


def hand_over(mixed_ref, log_ref, mixed_out_ref, log_out_ref):
    mixed_out_ref[...] = mixed_ref[...]
    log_out_ref[...] = log_ref[...]


def shards(tokens, w_query, w_key, w_value, w_output, query_gain, key_gain):
    vmem = pltpu.VMEM
    bf16, f32 = jnp.bfloat16, jnp.float32
    dma = pltpu.SemaphoreType.DMA
    hbm = pl.BlockSpec(memory_space=pl.ANY)
    local = pl.BlockSpec(memory_space=vmem)
    mixed_out, log_sums = pl.pallas_call(
        kernel,
        out_shape=(
            jax.ShapeDtypeStruct((OUT_ROWS, D), bf16),
            jax.ShapeDtypeStruct((4, ROWS), f32),
        ),
        in_specs=[hbm] * 5 + [local] * 2,
        out_specs=(local, local),
        scratch_shapes=[
            vmem((ROWS, D), bf16),
            vmem((D, 4 * HEAD), bf16),
            vmem((HEAD, D), bf16),
            vmem((HEAD, D), bf16),
            vmem((UNITS, HALF_ROWS, 2 * HEAD), bf16),
            vmem((2, 2 * HEAD, NQ), bf16),
            vmem((TP, 4 * HEAD, D), bf16),
            vmem((CH, 2 * HEAD), bf16),
            vmem((CH, 2 * HEAD), bf16),
            vmem((80, CH), bf16),
            vmem((80, CH), bf16),
            vmem((CH, QT), f32),
            vmem((CH, QT), f32),
            vmem((8, QT), f32),
            vmem((8, QT), f32),
            vmem((80, NQ), f32),
            vmem((80, NQ), f32),
            vmem((8, NQ), f32),
            vmem((8, NQ), f32),
            vmem((80, NQ), f32),
            vmem((8, NQ), f32),
            vmem((TP, OUT_ROWS, 4 * HEAD), bf16),
            vmem((TP, OUT_ROWS, 4 * HEAD), bf16),
            dma((5,)),
            dma((len(COPIES),)),
            dma((len(COPIES),)),
            dma((2,)),
            dma((2,)),
            dma((2,)),
            dma((TP,)),
            dma((TP,)),
            dma((7,)),
            dma((7,)),
        ],
        compiler_params=pltpu.CompilerParams(
            collective_id=0, has_side_effects=True, vmem_limit_bytes=58 << 20
        ),
        name="layer",
    )(
        tokens, w_query, w_key.T, w_value.T, w_output,
        query_gain.reshape(1, HEAD), key_gain.reshape(1, HEAD),
    )
    return pl.pallas_call(
        hand_over,
        out_shape=(
            jax.ShapeDtypeStruct(mixed_out.shape, mixed_out.dtype),
            jax.ShapeDtypeStruct(log_sums.shape, log_sums.dtype),
        ),
        in_specs=[local, local],
        out_specs=(local, local),
        name="hand_over",
    )(mixed_out, log_sums)


def solution(mesh):
    placed = (P("sp", None), P(None, "tp"), P(None, "tp"), P(None, "tp"), P("tp", None), P(), P())
    return jax.shard_map(
        shards,
        mesh=mesh,
        in_specs=placed,
        out_specs=(P(("sp", "tp"), None), P("tp", "sp")),
        check_vma=False,
    )
```
